32 devices in a mesh: fs: 8 (over z, y), tp: 4 (over x, core).
Axes of the slice: x: 2, y: 2, z: 4, core: 2. Of those that a mesh axis runs over, the one named last changes fastest.
Arguments:
- tokens: bfloat16 [4096, 4096], P('fs'), may hold values from -6 to 6
- norm_gain: float32 [4096], P('fs'), may hold values from 0.1 to 1.9
- gate_train: float32 [8, 4096, 1024], P(None, 'fs', 'tp'), may hold values from -0.09375 to 0.09375
- up_train: float32 [8, 4096, 1024], P(None, 'fs', 'tp'), may hold values from -0.09375 to 0.09375
- down_train: float32 [8, 1024, 4096], P(None, 'fs', 'tp'), may hold values from -0.1875 to 0.1875
- shared_gate_train: float32 [4096, 1024], P('fs', 'tp'), may hold values from -0.09375 to 0.09375
- shared_up_train: float32 [4096, 1024], P('fs', 'tp'), may hold values from -0.09375 to 0.09375
- shared_down_train: float32 [1024, 4096], P('fs', 'tp'), may hold values from -0.1875 to 0.1875
- route_expert: int32 [4096, 2], P('fs'), may hold values from 0 to 7, all different within a row; in each aligned block of 512 rows (0 to 511, 512 to 1023, ...) at most 192 rows name the same one
- route_weight: float32 [4096, 2], P('fs'), may hold values from 0.1 to 1
Outputs:
- expert_gate: bfloat16 [8, 4096, 1024], P('fs', None, 'tp')
- expert_up: bfloat16 [8, 4096, 1024], P('fs', None, 'tp')
- expert_down: bfloat16 [8, 1024, 4096], P('fs', 'tp')
- shared_gate: bfloat16 [4096, 1024], P(None, 'tp')
- shared_up: bfloat16 [4096, 1024], P(None, 'tp')
- shared_down: bfloat16 [1024, 4096], P('tp')
- mixed: bfloat16 [4096, 4096], P('fs', 'tp')
The draws below stay inside these ranges and needn't reach their ends.
Inputs may be any that keep to these rules, and one draw needn't show every extreme that they name: `route_expert`: each row names 2 different experts. Within each aligned block of 512 rows no expert is named by more than 192 rows, a bound that some block reaches in every draw.
All inputs are finite; a program needn't handle non-finite values.
Results may differ from the reference program's by a relative error of at most 0.015.
Values may be sent and summed in bfloat16 or wider, within the bound.
A program may use at most 128 MiB of HBM per device.

```python
import math
import jax
import jax.numpy as jnp
import numpy as np
from jax import lax

D = 4096
H = 1024
HS = 1024
TOPK = 2
TOK_DEV = 512
EXPERTS = 8
CAP = 192
TOKENS = 4096
N_FS = 8
N_TP = 4


def levels(rng, dims, shards, low, top_value):
    loudness = 1.0
    for axis_at, shards_of in shards:
        draws = jax.random.uniform(jax.random.fold_in(jax.random.fold_in(rng, 6), axis_at), (shards_of,), jnp.float32, low / len(shards), top_value / len(shards))
        loudness = loudness * jnp.repeat(jnp.exp(draws), dims[axis_at] // shards_of).reshape((-1,) + (1,) * (len(dims) - 1 - axis_at))
    return loudness


def shared_out(key, own, number, rows, amount, top, reach, lean):
    sequence = jax.random.permutation(key, amount)
    crowded, ordinary = shares(amount, rows * top, reach, lean, True), shares(amount, rows * top, reach, lean, False)
    places = jnp.arange(amount)

    def named(sizes, rotation):
        used = int((sizes > 0).sum())
        fixed = max(1, used // 4)
        shifted = fixed + (places - fixed + rotation * (used - fixed)) % max(1, amount - fixed)
        return jnp.zeros((amount,), jnp.int32).at[sequence[jnp.where(places < fixed, places, shifted)]].set(jnp.asarray(sizes, jnp.int32))

    sizes = jnp.where(number % 4 == 0, named(crowded, number // 4), named(ordinary, number - number // 4 - 1))
    mixed = jax.random.permutation(jax.random.fold_in(own, 3), amount)
    giver, taker = mixed[0:amount // 2 * 2:2], mixed[1:amount // 2 * 2:2]
    margin = jnp.minimum(sizes[giver] - 1, reach - sizes[taker]) // 2
    margin = jnp.where((giver == sequence[0]) | (taker == sequence[0]) | (sizes[taker] == 0), 0, jnp.maximum(margin, 0))
    shifted = jax.random.randint(jax.random.fold_in(own, 4), (amount // 2,), 0, 1 << 20) % (margin + 1)
    sizes = sizes.at[giver].add(-shifted).at[taker].add(shifted)
    labels = jnp.searchsorted(jnp.cumsum(sizes), jnp.arange(rows * top), side="right").astype(jnp.int32)
    table = labels.reshape(top, rows).T
    table = table[jax.random.permutation(jax.random.fold_in(own, 1), rows)]
    rotation = jax.random.randint(jax.random.fold_in(own, 2), (rows, 1), 0, top)
    return jnp.take_along_axis(table, (jnp.arange(top)[None, :] + rotation) % top, axis=1)


def shares(amount, total, reach, skew, full):
    portions = [(1 << 20) // math.isqrt(standing ** skew) + 1 for standing in range(1, amount + 1)]
    largest = reach if full else min(reach, max(-(-total // amount), total * portions[0] // sum(portions)))
    least = 1 if total - largest >= amount - 1 else 0
    holding, surplus = [largest] + [least] * (amount - 1), total - largest - least * (amount - 1)
    while surplus > 0:
        free = [i for i in range(1, amount) if holding[i] < largest] or [i for i in range(1, amount) if holding[i] < reach]
        whole, left = sum([portions[i] for i in free]), surplus
        for i in free:
            more = min(reach - holding[i], max(1, left * portions[i] // whole), surplus)
            holding[i] = holding[i] + more
            surplus = surplus - more
    return np.array(holding)


def noise(own_key, extent, spread, limit, shards=(), kind=jnp.bfloat16):
    loudness = levels(own_key, extent, shards, -0.22, 0.18) if shards else 1.0
    array = jax.random.normal(own_key, extent, jnp.float32) * spread * loudness
    return jnp.minimum(jnp.maximum(array, -limit), limit).astype(kind)


def setup_inputs(seed: int = 0) -> dict:
    keys = jax.random.split(jax.random.key(seed), 11)
    tokens = noise(keys[0], (TOKENS, D), 1.0, 6.0, ((0, 8),))
    norm_gain = jnp.clip(1.0 + 0.18 * jax.random.normal(keys[1], (D,), jnp.float32), 0.1, 1.9)
    gate_train = noise(keys[2], (EXPERTS, D, H), D ** -0.5, 0.09375, ((1, 8), (2, 4)), jnp.float32)
    up_train = noise(keys[3], (EXPERTS, D, H), D ** -0.5, 0.09375, ((1, 8), (2, 4)), jnp.float32)
    down_train = noise(keys[4], (EXPERTS, H, D), H ** -0.5, 0.1875, ((1, 8), (2, 4)), jnp.float32)
    shared_gate_train = noise(keys[5], (D, HS), D ** -0.5, 0.09375, ((0, 8), (1, 4)), jnp.float32)
    shared_up_train = noise(keys[6], (D, HS), D ** -0.5, 0.09375, ((0, 8), (1, 4)), jnp.float32)
    shared_down_train = noise(keys[7], (HS, D), HS ** -0.5, 0.1875, ((0, 8), (1, 4)), jnp.float32)
    route_expert_keys = jax.random.split(jax.random.fold_in(keys[8], 1), TOKENS // TOK_DEV)
    route_expert_turns = jax.random.permutation(jax.random.fold_in(keys[8], 3), TOKENS // TOK_DEV)
    route_expert = jax.vmap(lambda own, number: shared_out(jax.random.fold_in(keys[8], 2), own, number, TOK_DEV, EXPERTS, TOPK, CAP, 1))(route_expert_keys, route_expert_turns).reshape((TOKENS, TOPK))
    route_weight = jnp.clip(jnp.exp(math.log(1.0) - 2.3025851 * jax.random.uniform(keys[9], (TOKENS, TOPK), jnp.float32) ** levels(keys[9], (TOKENS, TOPK), ((0, 8),), -0.2, 0.2)), 0.1, 1.0)
    return {"tokens": tokens, "norm_gain": norm_gain, "gate_train": gate_train, "up_train": up_train, "down_train": down_train, "shared_gate_train": shared_gate_train, "shared_up_train": shared_up_train, "shared_down_train": shared_down_train, "route_expert": route_expert, "route_weight": route_weight}


norm_eps = 1e-06

def expert_apply(rows, weight_gate, weight_up, weight_down, pieces):
    gate_vals = jnp.dot(rows, weight_gate, preferred_element_type=jnp.float32)
    up_vals = jnp.dot(rows, weight_up, preferred_element_type=jnp.float32)
    hidden = (jax.nn.silu(gate_vals) * up_vals).astype(jnp.bfloat16)
    step_width = hidden.shape[1] // pieces
    total = jnp.zeros((rows.shape[0], weight_down.shape[1]), jnp.float32)
    for block in range(pieces):
        term = jnp.dot(hidden[:, block * step_width:(block + 1) * step_width], weight_down[block * step_width:(block + 1) * step_width], preferred_element_type=jnp.float32)
        total = total + term.astype(jnp.bfloat16).astype(jnp.float32)
    return total

def reference(tokens, norm_gain, gate_train, up_train, down_train, shared_gate_train, shared_up_train, shared_down_train, route_expert, route_weight):
    expert_gate = (norm_gain[None, :, None] * gate_train).astype(jnp.bfloat16)
    expert_up = (norm_gain[None, :, None] * up_train).astype(jnp.bfloat16)
    expert_down = down_train.astype(jnp.bfloat16)
    shared_gate = (norm_gain[:, None] * shared_gate_train).astype(jnp.bfloat16)
    shared_up = (norm_gain[:, None] * shared_up_train).astype(jnp.bfloat16)
    shared_down = shared_down_train.astype(jnp.bfloat16)
    values = tokens.astype(jnp.float32)
    normed = (values * lax.rsqrt(lax.optimization_barrier(jnp.mean(values * values, axis=1, keepdims=True)) + norm_eps)).astype(jnp.bfloat16)
    pairs = route_expert.reshape(N_FS, TOK_DEV * TOPK)
    chosen = (pairs[:, :, None] == jnp.arange(EXPERTS, dtype=jnp.int32)[None, None, :]).astype(jnp.int32)
    earlier = (jnp.cumsum(chosen, axis=1) - chosen).astype(jnp.int32)
    slot = lax.optimization_barrier(jnp.sum(earlier * chosen, axis=2)).astype(jnp.int32)
    place = (jnp.arange(N_FS, dtype=jnp.int32)[:, None] * CAP + slot).reshape(-1).astype(jnp.int32)
    expert_flat = route_expert.reshape(-1).astype(jnp.int32)
    token_of = (jnp.arange(TOKENS * TOPK, dtype=jnp.int32) // TOPK).astype(jnp.int32)
    table = jnp.zeros((EXPERTS, N_FS * CAP), jnp.int32).at[expert_flat, place].set(token_of)

    def one_expert(operands):
        row_index, weight_gate, weight_up, weight_down = operands
        rows = normed[row_index]
        return expert_apply(rows, weight_gate, weight_up, weight_down, N_TP).astype(jnp.bfloat16)
    results = lax.map(one_expert, (table, expert_gate, expert_up, expert_down))
    picked = results[expert_flat, place].reshape(TOKENS, TOPK, D)
    routed = lax.optimization_barrier(jnp.sum(route_weight[:, :, None] * picked.astype(jnp.float32), axis=1))
    shared_result = expert_apply(normed, shared_gate, shared_up, shared_down, N_TP)
    mixed = (routed + shared_result).astype(jnp.bfloat16)
    return (expert_gate, expert_up, expert_down, shared_gate, shared_up, shared_down, mixed)
```

```python
import jax
import jax.numpy as jnp
from jax import lax
from jax.sharding import PartitionSpec as P

norm_eps = 1e-06
chunks = 2
cores = 2


def regroup(experts, pieces, turn):
    per = experts // pieces
    return [
        (
            f * pieces + t,
            ((f % per * pieces + t + turn) % experts) * pieces + f // per,
        )
        for f in range(experts)
        for t in range(pieces)
    ]


def hop(values, pieces, across, swap):
    pairs = []
    for t in range(pieces):
        x, c = t // cores, t % cores
        far = (x + across) % (pieces // cores)
        pairs.append((t, far * cores + (cores - 1 - c if swap else c)))
    return lax.ppermute(values, "tp", pairs)


def gathered(own, pieces, tp_at):
    chips = pieces // cores
    x, c = tp_at // cores, tp_at % cores
    mine = [own] + [hop(own, pieces, s, False) for s in range(1, chips)]
    found = []
    for s, piece in enumerate(mine):
        at = (x - s) % chips * cores
        found.append((piece, at + c))
        found.append((hop(piece, pieces, 0, True), at + cores - 1 - c))
    return found


def scattered(hidden, weight, pieces, tp_at):
    chips = pieces // cores
    columns = weight.shape[1] // pieces
    x, c = tp_at // cores, tp_at % cores

    def term(at):
        block = lax.dynamic_slice_in_dim(weight, at * columns, columns, 1)
        return jnp.dot(hidden, block, preferred_element_type=jnp.float32)

    total = None
    for s in list(range(1, chips)) + [0]:
        at = (x + s) % chips * cores
        other = hop(term(at + cores - 1 - c).astype(jnp.bfloat16), pieces, 0, True)
        both = term(at + c) + other.astype(jnp.float32)
        if s:
            both = hop(both.astype(jnp.bfloat16), pieces, s, False).astype(jnp.float32)
        total = both if total is None else total + both
    return total


def on_device(
    tokens,
    norm_gain,
    gate_train,
    up_train,
    down_train,
    shared_gate_train,
    shared_up_train,
    shared_down_train,
    route_expert,
    route_weight,
):
    experts = lax.axis_size("fs")
    pieces = lax.axis_size("tp")
    fs_at = lax.axis_index("fs")
    tp_at = lax.axis_index("tp")
    per = experts // pieces
    tok_rows, model_width = tokens.shape
    top_count = route_expert.shape[1]
    capacity = 3 * tok_rows * top_count // (2 * experts)
    part = capacity // chunks
    columns = model_width // pieces

    gain_rows = norm_gain[None, :, None]
    gate_local = (gain_rows * gate_train).astype(jnp.bfloat16)
    up_local = (gain_rows * up_train).astype(jnp.bfloat16)
    expert_gate = lax.all_to_all(gate_local, "fs", split_axis=0, concat_axis=1, tiled=True)

    shared_width = shared_gate_train.shape[1]
    shared_local = (
        norm_gain[:, None] * jnp.concatenate([shared_gate_train, shared_up_train], axis=1)
    ).astype(jnp.bfloat16)
    shared_both = lax.all_gather(shared_local, "fs", axis=0, tiled=True)
    shared_down_own = lax.ppermute(
        shared_down_train.astype(jnp.bfloat16), ("fs", "tp"), regroup(experts, pieces, 0)
    )
    shared_down_all = lax.all_gather(shared_down_own, "fs", axis=0)
    depth, down_width = shared_down_train.shape
    shared_down = (
        shared_down_all.reshape(per, pieces, depth, down_width)
        .transpose(0, 2, 1, 3)
        .reshape(per * depth, pieces * down_width)
    )

    values = tokens.astype(jnp.float32)
    normed = (
        values * lax.rsqrt(jnp.mean(values * values, axis=1, keepdims=True) + norm_eps)
    ).astype(jnp.bfloat16)
    pairs = route_expert.reshape(-1)
    chosen = (pairs[:, None] == jnp.arange(experts, dtype=jnp.int32)[None, :]).astype(jnp.int32)
    earlier = jnp.cumsum(chosen, axis=0) - chosen
    slot_of = jnp.sum(earlier * chosen, axis=1)
    target = (slot_of // part) * (experts * part) + pairs * part + slot_of % part
    target = target.reshape(tok_rows, top_count)
    matches = target[:, :, None] == jnp.arange(experts * capacity, dtype=jnp.int32)[None, None, :]
    placing = jnp.sum(matches.astype(jnp.bfloat16), axis=1)
    weighing = jnp.sum(jnp.where(matches, route_weight[:, :, None], 0.0), axis=1).astype(
        jnp.bfloat16
    )
    own_columns = lax.dynamic_slice_in_dim(normed, tp_at * columns, columns, 1)
    span = experts * part
    arriving, behind = [], expert_gate
    for c in range(chunks):
        outgoing = jnp.einsum(
            "ts,td->sd",
            placing[:, c * span : (c + 1) * span],
            own_columns,
            preferred_element_type=jnp.float32,
        )
        outgoing = outgoing.astype(jnp.bfloat16).reshape(experts, part, columns)
        outgoing, behind = lax.optimization_barrier((outgoing, behind))
        if c == 0:
            expert_gate = behind
        behind = lax.all_to_all(outgoing, "fs", split_axis=0, concat_axis=0, tiled=True)
        arriving.append(behind)
    up_local, down_train, arriving[-1] = lax.optimization_barrier(
        (up_local, down_train, arriving[-1])
    )
    arrived = [gathered(a.reshape(span, columns), pieces, tp_at) for a in arriving]
    expert_up = lax.all_to_all(up_local, "fs", split_axis=0, concat_axis=1, tiled=True)

    expert_depth, expert_down_width = down_train.shape[1:]
    down_local = down_train.astype(jnp.bfloat16)
    in_group = fs_at % per * pieces + tp_at
    expert_down = jnp.zeros((per * expert_depth, pieces * expert_down_width), jnp.bfloat16)
    for turn in range(experts):
        block = lax.dynamic_index_in_dim(
            down_local, (in_group + turn) % experts, 0, keepdims=False
        )
        block = lax.ppermute(block, ("fs", "tp"), regroup(experts, pieces, turn))
        source = (fs_at - turn) % experts
        expert_down = lax.dynamic_update_slice(
            expert_down,
            block,
            (source // pieces * expert_depth, source % pieces * expert_down_width),
        )

    shared_vals = jnp.dot(normed, shared_both, preferred_element_type=jnp.float32)
    shared_hidden = (
        jax.nn.silu(shared_vals[:, :shared_width]) * shared_vals[:, shared_width:]
    ).astype(jnp.bfloat16)
    mixed = scattered(shared_hidden, shared_down, pieces, tp_at)

    sums = []
    for c in range(chunks):
        gate_vals, up_vals = 0.0, 0.0
        for piece, at in arrived[c]:
            gate_rows = lax.dynamic_slice_in_dim(expert_gate[0], at * columns, columns, 0)
            up_rows = lax.dynamic_slice_in_dim(expert_up[0], at * columns, columns, 0)
            gate_vals += jnp.dot(piece, gate_rows, preferred_element_type=jnp.float32)
            up_vals += jnp.dot(piece, up_rows, preferred_element_type=jnp.float32)
        hidden = (jax.nn.silu(gate_vals) * up_vals).astype(jnp.bfloat16)
        sums.append(scattered(hidden, expert_down, pieces, tp_at).astype(jnp.bfloat16))
    for c in range(chunks):
        returned = lax.all_to_all(
            sums[c].reshape(experts, part, columns), "fs", split_axis=0, concat_axis=0, tiled=True
        )
        mixed = mixed + jnp.dot(
            weighing[:, c * span : (c + 1) * span],
            returned.reshape(span, columns),
            preferred_element_type=jnp.float32,
        )
    return (
        expert_gate,
        expert_up,
        expert_down[None],
        shared_both[:, :shared_width],
        shared_both[:, shared_width:],
        shared_down,
        mixed.astype(jnp.bfloat16),
    )


def solution(mesh):
    placed = (
        P("fs", None),
        P("fs"),
        P(None, "fs", "tp"),
        P(None, "fs", "tp"),
        P(None, "fs", "tp"),
        P("fs", "tp"),
        P("fs", "tp"),
        P("fs", "tp"),
        P("fs", None),
        P("fs", None),
    )
    return jax.shard_map(
        on_device,
        mesh=mesh,
        in_specs=placed,
        out_specs=(
            P("fs", None, "tp"),
            P("fs", None, "tp"),
            P("fs", "tp", None),
            P(None, "tp"),
            P(None, "tp"),
            P("tp", None),
            P("fs", "tp"),
        ),
        check_vma=False,
    )
```
